32 devices in a mesh: rep: 2 (over x), fs: 8 (over z, y), tp: 2 (over core).
Axes of the slice: x: 2, y: 2, z: 4, core: 2. Of those that a mesh axis runs over, the one named last changes fastest.
Arguments:
- gate_late: bfloat16 [6144, 4096], P(('rep', 'fs'), 'tp'), may hold values from -6 to 6
- up_late: bfloat16 [6144, 4096], P(('rep', 'fs'), 'tp'), may hold values from -6 to 6
- gate_early: bfloat16 [6144, 4096], P(('rep', 'fs'), 'tp'), may hold values from -6 to 6
- up_early: bfloat16 [6144, 4096], P(('rep', 'fs'), 'tp'), may hold values from -6 to 6
- cotangent: bfloat16 [6144, 2048], P(('rep', 'fs')), may hold values from -6 to 6
- w_down: bfloat16 [2048, 4096], P('fs', 'tp'), may hold values from -0.09375 to 0.09375
- grad_in: float32 [2048, 4096], P('fs', 'tp'), may hold values from -6 to 6
Outputs:
- late_out: bfloat16 [6144, 2048], P(('rep', 'fs'))
- gate_grad: bfloat16 [6144, 4096], P(('rep', 'fs'), 'tp')
- up_grad: bfloat16 [6144, 4096], P(('rep', 'fs'), 'tp')
- grad_out: float32 [2048, 4096], P('fs', 'tp')
The draws below stay inside these ranges and needn't reach their ends.
All inputs are finite; a program needn't handle non-finite values.
Results may differ from the reference program's by a relative error of at most 0.014.
Values may be sent and summed in bfloat16 or wider, within the bound.
A program may use at most 64 MiB of HBM per device.

```python
import jax
import jax.numpy as jnp
from jax import lax

D = 2048
FF = 4096
TOKENS = 6144
N_TP = 2


def spiked(result, own_key, source, target, blocks, factor):
    def block_of(position):
        return (jnp.arange(result.shape[position]) // (result.shape[position] // blocks)).reshape((-1,) + (1,) * (result.ndim - 1 - position))

    one_side = jax.random.permutation(own_key, blocks)[block_of(target)]
    other_side = (block_of(target) + blocks // 2) % blocks
    return jnp.where((block_of(source) == one_side) | (block_of(source) == other_side), factor * result, result)


def steps_of(own_key, extent, shards, smallest, largest):
    gain = 1.0
    for position, blocks in shards:
        steps = jax.random.uniform(jax.random.fold_in(jax.random.fold_in(own_key, 6), position), (blocks,), jnp.float32, smallest / len(shards), largest / len(shards))
        gain = gain * jnp.repeat(jnp.exp(steps), extent[position] // blocks).reshape((-1,) + (1,) * (len(extent) - 1 - position))
    return gain


def normal_values(key, dims, deviation, limit, pieces=(), kind=jnp.bfloat16):
    loudness = steps_of(key, dims, pieces, -0.22, 0.18) if pieces else 1.0
    result = jax.random.normal(key, dims, jnp.float32) * deviation * loudness
    return jnp.minimum(jnp.maximum(result, -limit), limit).astype(kind)


def gaussian_with(stream_key, shape, width, reach, cuts, heavy, kind=jnp.bfloat16):
    drawn = width * jax.random.normal(stream_key, shape, jnp.float32)
    if cuts:
        drawn = drawn * steps_of(stream_key, shape, cuts, -0.22, 0.18)
    return jnp.clip(spiked(drawn, jax.random.fold_in(stream_key, 3), *heavy), -reach, reach).astype(kind)


def setup_inputs(seed: int = 0) -> dict:
    splits = jax.random.split(jax.random.key(seed), 8)
    return {
        "gate_late": normal_values(splits[0], (TOKENS, FF), 1.0, 6.0, ((0, 16), (1, 2))),
        "up_late": normal_values(splits[1], (TOKENS, FF), 1.0, 6.0, ((0, 16), (1, 2))),
        "gate_early": normal_values(splits[2], (TOKENS, FF), 1.0, 6.0, ((0, 16), (1, 2))),
        "up_early": normal_values(splits[3], (TOKENS, FF), 1.0, 6.0, ((0, 16), (1, 2))),
        "cotangent": gaussian_with(splits[4], (TOKENS, D), 1.0, 6.0, ((0, 16),), (0, 1, 16, 2.0)),
        "w_down": normal_values(splits[5], (D, FF), FF ** -0.5, 0.09375, ((0, 8), (1, 2))),
        "grad_in": normal_values(splits[6], (D, FF), 1.0, 6.0, ((0, 8), (1, 2)), jnp.float32),
    }


def reference(gate_late, up_late, gate_early, up_early, cotangent, w_down, grad_in):
    gate_value = gate_late.astype(jnp.float32)
    hidden_late = (jax.nn.silu(gate_value) * up_late.astype(jnp.float32)).astype(jnp.bfloat16)
    block_width = FF // N_TP

    def add_block(block_index, running):
        offset = (block_index * block_width).astype(jnp.int32)
        hidden_block = lax.dynamic_slice_in_dim(hidden_late, offset, block_width, 1)
        weight_block = lax.dynamic_slice_in_dim(w_down, offset, block_width, 1)
        partial_value = lax.dot_general(hidden_block, weight_block, (((1,), (1,)), ((), ())), preferred_element_type=jnp.float32)
        rounded = lax.optimization_barrier(partial_value.astype(jnp.bfloat16))
        return running + rounded.astype(jnp.float32)
    summed = lax.fori_loop(0, N_TP, add_block, jnp.zeros((gate_late.shape[0], D), jnp.float32))
    late_out = summed.astype(jnp.bfloat16)
    gate_value = gate_early.astype(jnp.float32)
    sigmoid_early = jax.nn.sigmoid(gate_value)
    swish_early = gate_value * sigmoid_early
    up_value = up_early.astype(jnp.float32)
    hidden_early = (swish_early * up_value).astype(jnp.bfloat16)
    hidden_grad = jnp.dot(cotangent, w_down, preferred_element_type=jnp.float32)
    gate_grad = (hidden_grad * up_value * sigmoid_early * (1.0 + gate_value * (1.0 - sigmoid_early))).astype(jnp.bfloat16)
    up_grad = (hidden_grad * swish_early).astype(jnp.bfloat16)
    weight_grad = lax.dot_general(cotangent, hidden_early, (((0,), (0,)), ((), ())), preferred_element_type=jnp.float32)
    grad_out = grad_in + weight_grad * (1.0 / jnp.sqrt(jnp.float32(TOKENS)))
    return (late_out, gate_grad, up_grad, grad_out)
```

```python
import functools
import math

import jax
import jax.numpy as jnp
from jax import lax
from jax.experimental import pallas as pl
from jax.experimental.pallas import tpu as pltpu
from jax.sharding import PartitionSpec as P

MESH = pl.DeviceIdType.MESH
F32 = jnp.float32
BF16 = jnp.bfloat16
LINK_ROWS = 16


def ring_place(index, count):
    odd = lax.rem(index, 2)
    half = lax.div(index, 2)
    return (1 - odd) * half + odd * (count - 1 - half)


def ring_index(place, count):
    place = lax.rem(place + 2 * count, count)
    back = lax.div(place, count // 2)
    return (1 - back) * 2 * place + back * (2 * (count - 1 - place) + 1)


def kernel(
    n, n_tp, qa, qr, scale,
    gl, ul, ge, ue, cot, cot_t, w, gin,
    late, gg, ug, gout,
    wf, lacc, hg, contrib, rs_s, rs_r, xr_s, xr_r, hl, he, part, fin_s, fin_r,
    ag_ss, ag_rs, xf_ss, xf_rs, rs_ss, rs_rs, xr_ss, xr_rs, fin_ss, fin_rs, tp_ss, tp_rs,
):
    tokens, cols = gl.shape
    rows = w.shape[0]
    half = cols // 2
    rep = lax.axis_index("rep")
    me = lax.axis_index("fs")
    tp = lax.axis_index("tp")
    place = ring_place(me, n)
    right = ring_index(place + 1, n)
    left = ring_index(place + n - 1, n)
    other = 1 - rep

    barrier = pltpu.get_barrier_semaphore()
    for target in (right, left):
        pl.semaphore_signal(barrier, inc=1, device_id={"fs": target}, device_id_type=MESH)
    pl.semaphore_signal(barrier, inc=1, device_id={"rep": other}, device_id_type=MESH)
    for k in range(1, n_tp):
        pl.semaphore_signal(
            barrier, inc=1, device_id={"tp": lax.rem(tp + k, n_tp)}, device_id_type=MESH
        )
    pl.semaphore_wait(barrier, 2 + n_tp)

    lanes = (pl.ds(0, half), pl.ds(half, half))
    towards = (right, left)

    def shard_at(way, step):
        return ring_index(place - step if way == 0 else place + step, n)

    def aligned(value):
        return pl.multiple_of(value, LINK_ROWS)

    ag_rows = pl.ds(aligned(rep * qa), rows - qa)
    ag_mine = pl.ds(aligned(rep * (rows - qa)), qa)
    ag_theirs = pl.ds(aligned(other * (rows - qa)), qa)
    rs_rows = pl.ds(aligned(rep * qr), rows - qr)
    rs_theirs = pl.ds(aligned(other * (rows - qr)), qr)
    rs_within = pl.ds(aligned(rep * (rows - 2 * qr)), qr)

    def gather(way, step, first=False):
        shard = shard_at(way, step)
        spot = wf.at[shard, ag_rows, lanes[way]]
        return pltpu.make_async_remote_copy(
            src_ref=w.at[ag_rows, lanes[way]] if first else spot,
            dst_ref=spot,
            send_sem=ag_ss.at[way, step],
            recv_sem=ag_rs.at[way, step],
            device_id={"fs": towards[way]},
            device_id_type=MESH,
        )

    def gather_wait(way, step):
        spot = wf.at[shard_at(way, step + 1), ag_rows, lanes[way]]
        pltpu.make_async_remote_copy(
            src_ref=spot, dst_ref=spot, send_sem=ag_ss.at[way, step],
            recv_sem=ag_rs.at[way, step], device_id={"fs": towards[way]}, device_id_type=MESH,
        ).wait_recv()

    def cross(way, step, span):
        spot = wf.at[shard_at(way, step + 1), span, lanes[way]]
        return pltpu.make_async_remote_copy(
            src_ref=spot, dst_ref=spot, send_sem=xf_ss.at[way, step],
            recv_sem=xf_rs.at[way, step], device_id={"rep": other}, device_id_type=MESH,
        )

    def reduce_copy(way, step):
        return pltpu.make_async_remote_copy(
            src_ref=rs_s.at[way, step], dst_ref=rs_r.at[way, step],
            send_sem=rs_ss.at[way, step], recv_sem=rs_rs.at[way, step],
            device_id={"fs": towards[way]}, device_id_type=MESH,
        )

    def pair_copy(way, step):
        return pltpu.make_async_remote_copy(
            src_ref=xr_s.at[way, step], dst_ref=xr_r.at[way, step],
            send_sem=xr_ss.at[way, step], recv_sem=xr_rs.at[way, step],
            device_id={"rep": other}, device_id_type=MESH,
        )

    for way in range(2):
        gather(way, 0, first=True).start()

    tile = 16

    @pl.loop(0, tokens // tile)
    def _(i):
        span = pl.ds(pl.multiple_of(i * tile, tile), tile)
        gate = ge[span, :].astype(F32)
        he[span, :] = (gate * (1.0 / (1.0 + jnp.exp(-gate))) * ue[span, :].astype(F32)).astype(BF16)

    def own_share(way, step):
        shard = shard_at(way, step + 1)
        contrib[way] = jnp.dot(cot_t[shard], he[:, lanes[way]], preferred_element_type=F32)
        xr_s[way, step] = contrib[way, rs_theirs, :].astype(BF16)
        pair_copy(way, step).start()

    def running(way, step):
        pair_copy(way, step).wait_recv()
        contrib[way, pl.ds(aligned(rep * (rows - qr)), qr), :] += xr_r[way, step].astype(F32)

    for way in range(2):
        own_share(way, 0)

    @pl.loop(0, tokens // tile)
    def _(i):
        span = pl.ds(pl.multiple_of(i * tile, tile), tile)
        gate = gl[span, :].astype(F32)
        hl[span, :] = (gate * (1.0 / (1.0 + jnp.exp(-gate))) * ul[span, :].astype(F32)).astype(BF16)
        hg[span, :] = jnp.zeros((tile, cols), F32)

    wf[me] = w[...]

    @pl.loop(0, n)
    def _(k):
        lacc[k] = jnp.zeros((tokens, rows), F32)

    for way in range(2):
        running(way, 0)
        rs_s[way, 0] = contrib[way, rs_rows, :].astype(BF16)
        reduce_copy(way, 0).start()

    def use(way, step):
        shard = shard_at(way, step)
        block = wf[shard, :, lanes[way]]
        lacc[shard] += lax.dot_general(
            hl[:, lanes[way]], block, (((1,), (1,)), ((), ())), preferred_element_type=F32
        )
        hg[:, lanes[way]] += jnp.dot(cot[shard], block, preferred_element_type=F32)

    def advance(step, last):
        for way in range(2):
            gather_wait(way, step)
            if not last:
                gather(way, step + 1).start()
            cross(way, step, ag_mine).start()
        for way in range(2):
            own_share(way, step + 1)
        for way in range(2):

            @pl.when(step >= 1)
            def _():
                cross(way, step - 1, ag_theirs).wait_recv()

            use(way, step)
        for way in range(2):
            running(way, step + 1)
            reduce_copy(way, step).wait_recv()
            total = contrib[way, rs_rows, :] + rs_r[way, step].astype(F32)
            if last:
                fin_s[:, lanes[way]] = total.astype(BF16)
            else:
                rs_s[way, step + 1] = total.astype(BF16)
                reduce_copy(way, step + 1).start()

    def body(step, carry):
        advance(step, False)
        return carry

    lax.fori_loop(0, n - 2, body, 0)
    advance(jnp.int32(n - 2), True)

    final = pltpu.make_async_remote_copy(
        src_ref=fin_s, dst_ref=fin_r, send_sem=fin_ss, recv_sem=fin_rs,
        device_id={"rep": other}, device_id_type=MESH,
    )
    final.start()

    for way in range(2):
        cross(way, n - 2, ag_theirs).wait_recv()
        use(way, n - 1)

    @pl.loop(0, n)
    def _(k):
        part[tp, k] = lacc[k].astype(BF16)

    def share(k):
        return pltpu.make_async_remote_copy(
            src_ref=part.at[tp], dst_ref=part.at[tp], send_sem=tp_ss.at[k], recv_sem=tp_rs.at[k],
            device_id={"tp": lax.rem(tp + k, n_tp)}, device_id_type=MESH,
        )

    def share_wait(k):
        spot = part.at[lax.rem(tp + n_tp - k, n_tp)]
        pltpu.make_async_remote_copy(
            src_ref=spot, dst_ref=spot, send_sem=tp_ss.at[k], recv_sem=tp_rs.at[k],
            device_id={"tp": lax.rem(tp + k, n_tp)}, device_id_type=MESH,
        ).wait_recv()

    for k in range(1, n_tp):
        share(k).start()

    @pl.loop(0, tokens // tile)
    def _(i):
        span = pl.ds(pl.multiple_of(i * tile, tile), tile)
        gate = ge[span, :].astype(F32)
        sig = 1.0 / (1.0 + jnp.exp(-gate))
        grad = hg[span, :]
        ug[span, :] = (grad * (gate * sig)).astype(BF16)
        gg[span, :] = (
            grad * ue[span, :].astype(F32) * sig * (1.0 + gate * (1.0 - sig))
        ).astype(BF16)

    for k in range(1, n_tp):
        share_wait(k)

    @pl.loop(0, n)
    def _(k):
        total = part[0, k].astype(F32)
        for j in range(1, n_tp):
            total = total + part[j, k].astype(F32)
        late[k] = total.astype(BF16)

    final.wait_recv()
    shared = rows - 2 * qr
    mine_only = pl.ds(aligned(rep * (rows - qr)), qr)
    theirs_only = pl.ds(aligned(other * (rows - qr)), qr)
    gout[mine_only, :] = gin[mine_only, :] + fin_s[rs_within, :].astype(F32) * scale
    gout[theirs_only, :] = (
        gin[theirs_only, :] + fin_r[pl.ds(aligned(other * shared), qr), :].astype(F32) * scale
    )
    both = pl.ds(qr, shared)
    gout[both, :] = gin[both, :] + scale * (
        fin_s[pl.ds(aligned(other * qr), shared), :].astype(F32)
        + fin_r[pl.ds(aligned(rep * qr), shared), :].astype(F32)
    )

    final.wait_send()
    for k in range(1, n_tp):
        share(k).wait_send()
    for way in range(2):
        gather(way, 0, first=True).wait_send()
        pair_copy(way, n - 1).wait_send()

    @pl.loop(0, n - 1)
    def _(step):
        for way in range(2):
            cross(way, step, ag_mine).wait_send()
            reduce_copy(way, step).wait_send()
            pair_copy(way, step).wait_send()

    @pl.loop(1, n - 1)
    def _(step):
        for way in range(2):
            gather(way, step).wait_send()


def solution(mesh):
    n, n_tp, n_rep = mesh.shape["fs"], mesh.shape["tp"], mesh.shape["rep"]
    assert n_rep == 2 and n % 2 == 0 and n > 2

    def per_device(gl, ul, ge, ue, cotangent, w, gin):
        tokens, cols = gl.shape
        rows, width = w.shape[0], cotangent.shape[1]
        half = cols // 2
        qa = (rows * 5 // 16) // LINK_ROWS * LINK_ROWS
        qr = (rows // 4) // LINK_ROWS * LINK_ROWS
        scale = 1.0 / math.sqrt(tokens * n_rep * n)
        cot = cotangent.reshape(tokens, n, rows).transpose(1, 0, 2)
        cot_t = cotangent.T.reshape(n, rows, tokens)
        vmem = pl.BlockSpec(memory_space=pltpu.VMEM)
        dma = pltpu.SemaphoreType.DMA
        late, gg, ug, gout = pl.pallas_call(
            functools.partial(kernel, n, n_tp, qa, qr, scale),
            out_shape=(
                jax.ShapeDtypeStruct((n, tokens, rows), BF16),
                jax.ShapeDtypeStruct((tokens, cols), BF16),
                jax.ShapeDtypeStruct((tokens, cols), BF16),
                jax.ShapeDtypeStruct((rows, cols), F32),
            ),
            in_specs=[vmem] * 8,
            out_specs=(vmem,) * 4,
            scratch_shapes=[
                pltpu.VMEM((n, rows, cols), BF16),
                pltpu.VMEM((n, tokens, rows), F32),
                pltpu.VMEM((tokens, cols), F32),
                pltpu.VMEM((2, rows, half), F32),
                pltpu.VMEM((2, n - 1, rows - qr, half), BF16),
                pltpu.VMEM((2, n - 1, rows - qr, half), BF16),
                pltpu.VMEM((2, n, qr, half), BF16),
                pltpu.VMEM((2, n, qr, half), BF16),
                pltpu.VMEM((tokens, cols), BF16),
                pltpu.VMEM((tokens, cols), BF16),
                pltpu.VMEM((n_tp, n, tokens, rows), BF16),
                pltpu.VMEM((rows - qr, cols), BF16),
                pltpu.VMEM((rows - qr, cols), BF16),
            ]
            + [dma((2, n))] * 8
            + [dma, dma, dma((n_tp,)), dma((n_tp,))],
            compiler_params=pltpu.CompilerParams(
                collective_id=0, has_side_effects=True, vmem_limit_bytes=67043328
            ),
        )(gl, ul, ge, ue, cot, cot_t, w, gin)
        return late.transpose(1, 0, 2).reshape(tokens, width), gg, ug, gout

    placed = (
        P(("rep", "fs"), "tp"),
        P(("rep", "fs"), "tp"),
        P(("rep", "fs"), "tp"),
        P(("rep", "fs"), "tp"),
        P(("rep", "fs"), None),
        P("fs", "tp"),
        P("fs", "tp"),
    )
    return jax.shard_map(
        per_device,
        mesh=mesh,
        in_specs=placed,
        out_specs=(
            P(("rep", "fs"), None),
            P(("rep", "fs"), "tp"),
            P(("rep", "fs"), "tp"),
            P("fs", "tp"),
        ),
        check_vma=False,
    )
```

```python
import functools
import math

import jax
import jax.numpy as jnp
from jax import lax
from jax.experimental import pallas as pl
from jax.experimental.pallas import tpu as pltpu
from jax.sharding import PartitionSpec as P

MESH = pl.DeviceIdType.MESH
F32 = jnp.float32
BF16 = jnp.bfloat16
LINK_ROWS = 16


def ring_place(index, count):
    odd = lax.rem(index, 2)
    half = lax.div(index, 2)
    return (1 - odd) * half + odd * (count - 1 - half)


def ring_index(place, count):
    place = lax.rem(place + 2 * count, count)
    back = lax.div(place, count // 2)
    return (1 - back) * 2 * place + back * (2 * (count - 1 - place) + 1)


def kernel(
    n, n_tp, qa, qr, scale,
    gl, ul, ge, ue, cot, w, gin,
    late, gg, ug, gout,
    wf, lacc, hg, contrib, rs_s, rs_r, xr_s, xr_r, hl, he, part, fin_s, fin_r,
    ag_ss, ag_rs, xf_ss, xf_rs, rs_ss, rs_rs, xr_ss, xr_rs, fin_ss, fin_rs, tp_ss, tp_rs,
):
    tokens, cols = gl.shape
    rows = w.shape[0]
    half = cols // 2
    rep = lax.axis_index("rep")
    me = lax.axis_index("fs")
    tp = lax.axis_index("tp")
    place = ring_place(me, n)
    right = ring_index(place + 1, n)
    left = ring_index(place + n - 1, n)
    other = 1 - rep

    barrier = pltpu.get_barrier_semaphore()
    for target in (right, left):
        pl.semaphore_signal(barrier, inc=1, device_id={"fs": target}, device_id_type=MESH)
    pl.semaphore_signal(barrier, inc=1, device_id={"rep": other}, device_id_type=MESH)
    for k in range(1, n_tp):
        pl.semaphore_signal(
            barrier, inc=1, device_id={"tp": lax.rem(tp + k, n_tp)}, device_id_type=MESH
        )
    pl.semaphore_wait(barrier, 2 + n_tp)

    lanes = (pl.ds(0, half), pl.ds(half, half))
    towards = (right, left)

    def shard_at(way, step):
        return ring_index(place - step if way == 0 else place + step, n)

    def columns(ref, shard):
        if len(ref.shape) == 3:
            return ref[shard]
        return ref[:, pl.ds(pl.multiple_of(shard * rows, rows), rows)]

    def aligned(value):
        return pl.multiple_of(value, LINK_ROWS)

    ag_rows = pl.ds(aligned(rep * qa), rows - qa)
    ag_mine = pl.ds(aligned(rep * (rows - qa)), qa)
    ag_theirs = pl.ds(aligned(other * (rows - qa)), qa)
    rs_rows = pl.ds(aligned(rep * qr), rows - qr)
    rs_theirs = pl.ds(aligned(other * (rows - qr)), qr)
    rs_within = pl.ds(aligned(rep * (rows - 2 * qr)), qr)

    def gather(way, step, first=False):
        shard = shard_at(way, step)
        spot = wf.at[shard, ag_rows, lanes[way]]
        return pltpu.make_async_remote_copy(
            src_ref=w.at[ag_rows, lanes[way]] if first else spot,
            dst_ref=spot,
            send_sem=ag_ss.at[way, step],
            recv_sem=ag_rs.at[way, step],
            device_id={"fs": towards[way]},
            device_id_type=MESH,
        )

    def gather_wait(way, step):
        spot = wf.at[shard_at(way, step + 1), ag_rows, lanes[way]]
        pltpu.make_async_remote_copy(
            src_ref=spot, dst_ref=spot, send_sem=ag_ss.at[way, step],
            recv_sem=ag_rs.at[way, step], device_id={"fs": towards[way]}, device_id_type=MESH,
        ).wait_recv()

    def cross(way, step, span):
        spot = wf.at[shard_at(way, step + 1), span, lanes[way]]
        return pltpu.make_async_remote_copy(
            src_ref=spot, dst_ref=spot, send_sem=xf_ss.at[way, step],
            recv_sem=xf_rs.at[way, step], device_id={"rep": other}, device_id_type=MESH,
        )

    def reduce_copy(way, step):
        return pltpu.make_async_remote_copy(
            src_ref=rs_s.at[way, step], dst_ref=rs_r.at[way, step],
            send_sem=rs_ss.at[way, step], recv_sem=rs_rs.at[way, step],
            device_id={"fs": towards[way]}, device_id_type=MESH,
        )

    def pair_copy(way, step):
        return pltpu.make_async_remote_copy(
            src_ref=xr_s.at[way, step], dst_ref=xr_r.at[way, step],
            send_sem=xr_ss.at[way, step], recv_sem=xr_rs.at[way, step],
            device_id={"rep": other}, device_id_type=MESH,
        )

    for way in range(2):
        gather(way, 0, first=True).start()

    tile = 16

    @pl.loop(0, tokens // tile)
    def _(i):
        span = pl.ds(pl.multiple_of(i * tile, tile), tile)
        gate = ge[span, :].astype(F32)
        he[span, :] = (gate * (1.0 / (1.0 + jnp.exp(-gate))) * ue[span, :].astype(F32)).astype(BF16)

    def own_share(way, step):
        shard = shard_at(way, step + 1)
        contrib[way] = lax.dot_general(
            columns(cot, shard), he[:, lanes[way]], (((0,), (0,)), ((), ())),
            preferred_element_type=F32,
        )
        xr_s[way, step] = contrib[way, rs_theirs, :].astype(BF16)
        pair_copy(way, step).start()

    def running(way, step):
        pair_copy(way, step).wait_recv()
        contrib[way, pl.ds(aligned(rep * (rows - qr)), qr), :] += xr_r[way, step].astype(F32)

    for way in range(2):
        own_share(way, 0)

    @pl.loop(0, tokens // tile)
    def _(i):
        span = pl.ds(pl.multiple_of(i * tile, tile), tile)
        gate = gl[span, :].astype(F32)
        hl[span, :] = (gate * (1.0 / (1.0 + jnp.exp(-gate))) * ul[span, :].astype(F32)).astype(BF16)
        hg[span, :] = jnp.zeros((tile, cols), F32)

    wf[me] = w[...]

    @pl.loop(0, n)
    def _(k):
        lacc[k] = jnp.zeros((tokens, rows), F32)

    for way in range(2):
        running(way, 0)
        rs_s[way, 0] = contrib[way, rs_rows, :].astype(BF16)
        reduce_copy(way, 0).start()

    def use(way, step):
        shard = shard_at(way, step)
        block = wf[shard, :, lanes[way]]
        lacc[shard] += lax.dot_general(
            hl[:, lanes[way]], block, (((1,), (1,)), ((), ())), preferred_element_type=F32
        )
        hg[:, lanes[way]] += jnp.dot(columns(cot, shard), block, preferred_element_type=F32)

    final = pltpu.make_async_remote_copy(
        src_ref=fin_s, dst_ref=fin_r, send_sem=fin_ss, recv_sem=fin_rs,
        device_id={"rep": other}, device_id_type=MESH,
    )

    def advance(step, last):
        for way in range(2):
            own_share(way, step + 1)
        for way in range(2):
            running(way, step + 1)
            reduce_copy(way, step).wait_recv()
            total = contrib[way, rs_rows, :] + rs_r[way, step].astype(F32)
            if last:
                fin_s[:, lanes[way]] = total.astype(BF16)
            else:
                rs_s[way, step + 1] = total.astype(BF16)
                reduce_copy(way, step + 1).start()
        if last:
            final.start()
        for way in range(2):

            @pl.when(step >= 1)
            def _():
                cross(way, step - 1, ag_theirs).wait_recv()

            use(way, step)
        for way in range(2):
            gather_wait(way, step)
            if not last:
                gather(way, step + 1).start()
            cross(way, step, ag_mine).start()

    def body(step, carry):
        advance(step, False)
        return carry

    lax.fori_loop(0, n - 2, body, 0)
    advance(jnp.int32(n - 2), True)

    for way in range(2):
        cross(way, n - 2, ag_theirs).wait_recv()
        use(way, n - 1)

    @pl.loop(0, n)
    def _(k):
        part[tp, k] = lacc[k].astype(BF16)

    def share(k):
        return pltpu.make_async_remote_copy(
            src_ref=part.at[tp], dst_ref=part.at[tp], send_sem=tp_ss.at[k], recv_sem=tp_rs.at[k],
            device_id={"tp": lax.rem(tp + k, n_tp)}, device_id_type=MESH,
        )

    def share_wait(k):
        spot = part.at[lax.rem(tp + n_tp - k, n_tp)]
        pltpu.make_async_remote_copy(
            src_ref=spot, dst_ref=spot, send_sem=tp_ss.at[k], recv_sem=tp_rs.at[k],
            device_id={"tp": lax.rem(tp + k, n_tp)}, device_id_type=MESH,
        ).wait_recv()

    for k in range(1, n_tp):
        share(k).start()

    @pl.loop(0, tokens // tile)
    def _(i):
        span = pl.ds(pl.multiple_of(i * tile, tile), tile)
        gate = ge[span, :].astype(F32)
        sig = 1.0 / (1.0 + jnp.exp(-gate))
        grad = hg[span, :]
        ug[span, :] = (grad * (gate * sig)).astype(BF16)
        gg[span, :] = (
            grad * ue[span, :].astype(F32) * sig * (1.0 + gate * (1.0 - sig))
        ).astype(BF16)

    for k in range(1, n_tp):
        share_wait(k)

    @pl.loop(0, n)
    def _(k):
        total = part[0, k].astype(F32)
        for j in range(1, n_tp):
            total = total + part[j, k].astype(F32)
        if len(late.shape) == 3:
            late[k] = total.astype(BF16)
        else:
            late[:, pl.ds(pl.multiple_of(k * rows, rows), rows)] = total.astype(BF16)

    final.wait_recv()
    shared = rows - 2 * qr
    mine_only = pl.ds(aligned(rep * (rows - qr)), qr)
    theirs_only = pl.ds(aligned(other * (rows - qr)), qr)
    gout[mine_only, :] = gin[mine_only, :] + fin_s[rs_within, :].astype(F32) * scale
    gout[theirs_only, :] = (
        gin[theirs_only, :] + fin_r[pl.ds(aligned(other * shared), qr), :].astype(F32) * scale
    )
    if shared:
        both = pl.ds(qr, shared)
        gout[both, :] = gin[both, :] + scale * (
            fin_s[pl.ds(aligned(other * qr), shared), :].astype(F32)
            + fin_r[pl.ds(aligned(rep * qr), shared), :].astype(F32)
        )

    final.wait_send()
    for k in range(1, n_tp):
        share(k).wait_send()
    for way in range(2):
        gather(way, 0, first=True).wait_send()
        pair_copy(way, n - 1).wait_send()

    @pl.loop(0, n - 1)
    def _(step):
        for way in range(2):
            cross(way, step, ag_mine).wait_send()
            reduce_copy(way, step).wait_send()
            pair_copy(way, step).wait_send()

    @pl.loop(1, n - 1)
    def _(step):
        for way in range(2):
            gather(way, step).wait_send()


def solution(mesh):
    n, n_tp, n_rep = mesh.shape["fs"], mesh.shape["tp"], mesh.shape["rep"]
    assert n_rep == 2 and n % 2 == 0 and n > 2

    def per_device(gl, ul, ge, ue, cotangent, w, gin):
        tokens, cols = gl.shape
        rows, width = w.shape[0], cotangent.shape[1]
        half = cols // 2
        qa = (rows * 3 // 16) // LINK_ROWS * LINK_ROWS
        qr = (rows * 6 // 16) // LINK_ROWS * LINK_ROWS
        scale = 1.0 / math.sqrt(tokens * n_rep * n)
        whole_lanes = rows % 128 == 0
        cot = cotangent
        if not whole_lanes:
            cot = cotangent.reshape(tokens, n, rows).transpose(1, 0, 2)
        vmem = pl.BlockSpec(memory_space=pltpu.VMEM)
        dma = pltpu.SemaphoreType.DMA
        late, gg, ug, gout = pl.pallas_call(
            functools.partial(kernel, n, n_tp, qa, qr, scale),
            out_shape=(
                jax.ShapeDtypeStruct(cot.shape, BF16),
                jax.ShapeDtypeStruct((tokens, cols), BF16),
                jax.ShapeDtypeStruct((tokens, cols), BF16),
                jax.ShapeDtypeStruct((rows, cols), F32),
            ),
            in_specs=[vmem] * 7,
            out_specs=(vmem,) * 4,
            scratch_shapes=[
                pltpu.VMEM((n, rows, cols), BF16),
                pltpu.VMEM((n, tokens, rows), F32),
                pltpu.VMEM((tokens, cols), F32),
                pltpu.VMEM((2, rows, half), F32),
                pltpu.VMEM((2, n - 1, rows - qr, half), BF16),
                pltpu.VMEM((2, n - 1, rows - qr, half), BF16),
                pltpu.VMEM((2, n, qr, half), BF16),
                pltpu.VMEM((2, n, qr, half), BF16),
                pltpu.VMEM((tokens, cols), BF16),
                pltpu.VMEM((tokens, cols), BF16),
                pltpu.VMEM((n_tp, n, tokens, rows), BF16),
                pltpu.VMEM((rows - qr, cols), BF16),
                pltpu.VMEM((rows - qr, cols), BF16),
            ]
            + [dma((2, n))] * 8
            + [dma, dma, dma((n_tp,)), dma((n_tp,))],
            compiler_params=pltpu.CompilerParams(
                collective_id=0, has_side_effects=True, vmem_limit_bytes=67043328
            ),
        )(gl, ul, ge, ue, cot, w, gin)
        if not whole_lanes:
            late = late.transpose(1, 0, 2).reshape(tokens, width)
        return late, gg, ug, gout

    placed = (
        P(("rep", "fs"), "tp"),
        P(("rep", "fs"), "tp"),
        P(("rep", "fs"), "tp"),
        P(("rep", "fs"), "tp"),
        P(("rep", "fs"), None),
        P("fs", "tp"),
        P("fs", "tp"),
    )
    return jax.shard_map(
        per_device,
        mesh=mesh,
        in_specs=placed,
        out_specs=(
            P(("rep", "fs"), None),
            P(("rep", "fs"), "tp"),
            P(("rep", "fs"), "tp"),
            P("fs", "tp"),
        ),
        check_vma=False,
    )
```
